32 devices in a mesh: grp: 2 (over y), fs: 8 (over z, core), tp: 2 (over x).
Axes of the slice: x: 2, y: 2, z: 4, core: 2. Of those that a mesh axis runs over, the one named last changes fastest.
Arguments:
- tokens: bfloat16 [3584, 2048], P(('grp', 'fs'), 'tp'), parts along dimension 0, may hold values from -170 to 170
- routes: int32 [3584, 6], P(('grp', 'fs')), parts along dimension 0, may hold values from 0 to 15, all different within a row; in each aligned block of 224 rows (0 to 223, 224 to 447, ...) at most 112 rows name the same one
- route_weights: float32 [3584, 6], P(('grp', 'fs')), parts along dimension 0, may hold values from 0.2 to 1
- norm_gain: float32 [2048], P('fs'), may hold values from 0.1 to 1.9
- gate_experts: float32 [16, 2048, 512], P(None, 'fs', 'tp'), may hold values from -0.125 to 0.125
- up_experts: float32 [16, 2048, 512], P(None, 'fs', 'tp'), may hold values from -0.125 to 0.125
- down_experts: float32 [16, 512, 2048], P(None, 'fs', 'tp'), may hold values from -0.25 to 0.25
- shared_gate: float32 [2048, 512], P('fs', 'tp'), may hold values from -0.125 to 0.125
- shared_up: float32 [2048, 512], P('fs', 'tp'), may hold values from -0.125 to 0.125
- shared_down: float32 [512, 2048], P('fs', 'tp'), may hold values from -0.25 to 0.25
Outputs:
- mixed: bfloat16 [3584, 2048], P(('grp', 'fs'), 'tp'), parts along dimension 0
- gate_ready: bfloat16 [32, 2048, 512], P(('grp', 'fs'), None, 'tp'), parts along dimension 0
- up_ready: bfloat16 [32, 2048, 512], P(('grp', 'fs'), None, 'tp'), parts along dimension 0
- down_ready: bfloat16 [32, 512, 2048], P(('grp', 'fs'), 'tp'), parts along dimension 0
- shared_gate_ready: bfloat16 [4096, 512], P('grp', 'tp'), parts along dimension 0
- shared_up_ready: bfloat16 [4096, 512], P('grp', 'tp'), parts along dimension 0
- shared_down_ready: bfloat16 [1024, 2048], P(('grp', 'tp')), parts along dimension 0
The draws below stay inside these ranges and needn't reach their ends.
There are 2 independent parts, one for each index of `grp`. The reference program is written for one: setup_inputs(seed, part) draws one part's arguments, and reference() takes and returns one part's arrays. A program takes and returns all parts, laid end to end along the dimension named above; an argument that names none is the same for every part. Nothing has to cross between parts.
Inputs may be any that keep to these rules, and one draw needn't show every extreme that they name: `routes`: the 6 experts of a row differ; among the rows of one index of fs no expert is named more than 112 times, a bound that some block reaches.
All inputs are finite; a program needn't handle non-finite values.
Results may differ from the reference program's by a relative error of at most 0.013.
Values may be sent and summed in bfloat16 or wider, within the bound.
A program may use at most 128 MiB of HBM per device.

```python
import math
import jax
import jax.numpy as jnp
import numpy as np
from jax import lax

D = 2048
FF = 512
SF = 512
EXPERTS = 16
TOP_K = 6
TOK_DEV = 224
TOKENS = 1792
CAP = 112
N_TP = 2


def draw_tokens(key, part):
    key_rows = jax.random.fold_in(key, 11)
    key_cols = jax.random.fold_in(key, 12)
    key_base = jax.random.fold_in(key, 13)
    row_scale = jnp.exp(jax.random.uniform(key_rows, (TOKENS, 1), jnp.float32, 0.0, math.log(10.0)))
    col_scale = jnp.exp(jax.random.uniform(key_cols, (1, D), jnp.float32, 0.0, math.log(10.0)))
    base = jnp.clip(jax.random.normal(key_base, (TOKENS, D), jnp.float32), -5.0, 5.0)
    return (base * row_scale * col_scale / 3.0).astype(jnp.bfloat16)


def block_scale(own_key, dims, cuts, low, top_value):
    def one(dim, blocks):
        steps = jax.random.uniform(jax.random.fold_in(jax.random.fold_in(own_key, 6), dim), (blocks,), jnp.float32, low / len(cuts), top_value / len(cuts))
        return jnp.repeat(jnp.exp(steps), dims[dim] // blocks).reshape((-1,) + (1,) * (len(dims) - dim - 1))

    gain = one(*cuts[0])
    for cut in cuts[1:]:
        gain = gain * one(*cut)
    return gain


def shared_out(rng, own, number, rows, amount, top, most, slope):
    order = jax.random.permutation(rng, amount)
    heavy_load, common = portions_of(amount, rows * top, most, slope, True), portions_of(amount, rows * top, most, slope, False)
    places = jnp.arange(amount)

    def named(lengths, turn):
        used = int((lengths > 0).sum())
        fixed = max(1, used // 4)
        passed = fixed + (places - fixed + turn * (used - fixed)) % max(1, amount - fixed)
        return jnp.zeros((amount,), jnp.int32).at[order[jnp.where(places < fixed, places, passed)]].set(jnp.asarray(lengths, jnp.int32))

    lengths = jnp.where(number % 4 == 0, named(heavy_load, number // 4), named(common, number - number // 4 - 1))
    mixed = jax.random.permutation(jax.random.fold_in(own, 3), amount)
    giver, receiver = mixed[0:amount // 2 * 2:2], mixed[1:amount // 2 * 2:2]
    room = jnp.minimum(lengths[giver] - 1, most - lengths[receiver]) // 2
    room = jnp.where((giver == order[0]) | (receiver == order[0]) | (lengths[receiver] == 0), 0, jnp.maximum(room, 0))
    passed = jax.random.randint(jax.random.fold_in(own, 4), (amount // 2,), 0, 1 << 20) % (room + 1)
    lengths = lengths.at[giver].add(-passed).at[receiver].add(passed)
    members = jnp.searchsorted(jnp.cumsum(lengths), jnp.arange(rows * top), side="right").astype(jnp.int32)
    grid = members.reshape(top, rows).T
    grid = grid[jax.random.permutation(jax.random.fold_in(own, 1), rows)]
    turn = jax.random.randint(jax.random.fold_in(own, 2), (rows, 1), 0, top)
    return jnp.take_along_axis(grid, (jnp.arange(top)[None, :] + turn) % top, axis=1)


def portions_of(amount, total, reach, skew, full):
    portions = [(1 << 20) // math.isqrt(rank ** skew) + 1 for rank in range(1, amount + 1)]
    largest = reach if full else min(reach, max(-(-total // amount), total * portions[0] // sum(portions)))
    least = 1 if total - largest >= amount - 1 else 0
    counts, spare = [largest] + [least] * (amount - 1), total - largest - least * (amount - 1)
    while spare > 0:
        movable = [i for i in range(1, amount) if counts[i] < largest] or [i for i in range(1, amount) if counts[i] < reach]
        pool, left = sum([portions[i] for i in movable]), spare
        for i in movable:
            addition = min(reach - counts[i], max(1, left * portions[i] // pool), spare)
            counts[i] = counts[i] + addition
            spare = spare - addition
    return np.array(counts)


def normal_values(stream_key, shape, scale, most, pieces=(), kind=jnp.bfloat16):
    factor_of = block_scale(stream_key, shape, pieces, -0.22, 0.18) if pieces else 1.0
    array = jax.random.normal(stream_key, shape, jnp.float32) * scale * factor_of
    return jnp.minimum(jnp.maximum(array, -most), most).astype(kind)


def setup_inputs(seed: int = 0, part: int = 0) -> dict:
    splits = jax.random.split(jax.random.key(seed), 11)
    part_splits = jax.random.split(jax.random.fold_in(splits[10], part), 11)
    tokens = draw_tokens(jax.random.fold_in(jax.random.fold_in(splits[10], part), 71), part)
    routes_keys = jax.random.split(jax.random.fold_in(part_splits[1], 1), TOKENS // TOK_DEV)
    routes_turns = jax.random.permutation(jax.random.fold_in(part_splits[1], 3), TOKENS // TOK_DEV)
    routes = jax.vmap(lambda own, number: shared_out(jax.random.fold_in(part_splits[1], 2), own, number, TOK_DEV, EXPERTS, TOP_K, CAP, 1))(routes_keys, routes_turns).reshape((TOKENS, TOP_K))
    route_weights = jnp.clip(jnp.exp(math.log(1.0) - 1.609438 * jax.random.uniform(part_splits[2], (TOKENS, TOP_K), jnp.float32) ** block_scale(part_splits[2], (TOKENS, TOP_K), ((0, 8),), -0.2, 0.2)), 0.2, 1.0)
    norm_gain = jnp.clip(1.0 + 0.18 * jax.random.normal(splits[3], (D,), jnp.float32), 0.1, 1.9)
    gate_experts = normal_values(splits[4], (EXPERTS, D, FF), D ** -0.5, 0.125, ((1, 8), (2, 2)), jnp.float32)
    up_experts = normal_values(splits[5], (EXPERTS, D, FF), D ** -0.5, 0.125, ((1, 8), (2, 2)), jnp.float32)
    down_experts = normal_values(splits[6], (EXPERTS, FF, D), FF ** -0.5, 0.25, ((1, 8), (2, 2)), jnp.float32)
    shared_gate = normal_values(splits[7], (D, SF), D ** -0.5, 0.125, ((0, 8), (1, 2)), jnp.float32)
    shared_up = normal_values(splits[8], (D, SF), D ** -0.5, 0.125, ((0, 8), (1, 2)), jnp.float32)
    shared_down = normal_values(splits[9], (SF, D), SF ** -0.5, 0.25, ((0, 8), (1, 2)), jnp.float32)
    return {"tokens": tokens, "routes": routes, "route_weights": route_weights, "norm_gain": norm_gain, "gate_experts": gate_experts, "up_experts": up_experts, "down_experts": down_experts, "shared_gate": shared_gate, "shared_up": shared_up, "shared_down": shared_down}


def grouped_product(active, weight):
    groups = N_TP
    span_cols = active.shape[1] // groups
    totals = jnp.zeros((active.shape[0], weight.shape[1]), jnp.float32)
    for section in range(groups):
        product = jnp.dot(active[:, section * span_cols:(section + 1) * span_cols], weight[section * span_cols:(section + 1) * span_cols], preferred_element_type=jnp.float32)
        rounded = lax.optimization_barrier(product.astype(jnp.bfloat16))
        totals = totals + rounded.astype(jnp.float32)
    return totals

def reference(tokens, routes, route_weights, norm_gain, gate_experts, up_experts, down_experts, shared_gate, shared_up, shared_down):
    gate_ready = (gate_experts * norm_gain[None, :, None]).astype(jnp.bfloat16)
    up_ready = (up_experts * norm_gain[None, :, None]).astype(jnp.bfloat16)
    down_ready = down_experts.astype(jnp.bfloat16)
    shared_gate_ready = (shared_gate * norm_gain[:, None]).astype(jnp.bfloat16)
    shared_up_ready = (shared_up * norm_gain[:, None]).astype(jnp.bfloat16)
    shared_down_ready = shared_down.astype(jnp.bfloat16)
    widened = tokens.astype(jnp.float32)
    normed = (widened * lax.rsqrt(lax.optimization_barrier(jnp.mean(widened * widened, axis=1, keepdims=True)) + 1e-06)).astype(jnp.bfloat16)
    shared_active = (jax.nn.silu(jnp.dot(normed, shared_gate_ready, preferred_element_type=jnp.float32)) * jnp.dot(normed, shared_up_ready, preferred_element_type=jnp.float32)).astype(jnp.bfloat16)
    shared_rows = grouped_product(shared_active, shared_down_ready)
    blocks = TOKENS // TOK_DEV
    pairs = TOK_DEV * TOP_K
    block_routes = routes.reshape(blocks, pairs)
    onehot = (block_routes[:, :, None] == jnp.arange(EXPERTS, dtype=jnp.int32)[None, None, :]).astype(jnp.int32)
    earlier = jnp.cumsum(onehot, axis=1) - onehot
    slot_index = lax.optimization_barrier(jnp.sum(earlier * onehot, axis=2)).astype(jnp.int32)
    target = block_routes * CAP + slot_index
    token_index = (jnp.arange(TOKENS * TOP_K, dtype=jnp.int32) // TOP_K).astype(jnp.int32)
    flat_target = (target + (jnp.arange(blocks, dtype=jnp.int32) * (EXPERTS * CAP))[:, None]).reshape(-1)
    source = jnp.full((blocks * EXPERTS * CAP,), -1, jnp.int32).at[flat_target].set(token_index)
    source = source.reshape(blocks, EXPERTS, CAP).transpose(1, 0, 2).reshape(EXPERTS, blocks * CAP)

    def expert_rows(operands):
        row_index, gate_one, up_one, down_one = operands
        present = row_index >= 0
        inputs = jnp.where(present[:, None], normed[jnp.maximum(row_index, 0)], jnp.zeros((), jnp.bfloat16))
        active = (jax.nn.silu(jnp.dot(inputs, gate_one, preferred_element_type=jnp.float32)) * jnp.dot(inputs, up_one, preferred_element_type=jnp.float32)).astype(jnp.bfloat16)
        return grouped_product(active, down_one).astype(jnp.bfloat16)
    results = lax.map(expert_rows, (source, gate_ready, up_ready, down_ready))
    flat_results = results.reshape(EXPERTS * blocks * CAP, D)
    block_of = (jnp.arange(TOKENS, dtype=jnp.int32) // TOK_DEV)[:, None]
    position = routes * (blocks * CAP) + block_of * CAP + slot_index.reshape(TOKENS, TOP_K)
    mixed = shared_rows
    for choice_k in range(TOP_K):
        mixed = mixed + flat_results[position[:, choice_k]].astype(jnp.float32) * route_weights[:, choice_k:choice_k + 1]
    return (mixed.astype(jnp.bfloat16), gate_ready, up_ready, down_ready, shared_gate_ready, shared_up_ready, shared_down_ready)
```

```python
import functools

import jax
import jax.numpy as jnp
from jax import lax
from jax.experimental import pallas as pl
from jax.experimental.pallas import tpu as pltpu
from jax.sharding import PartitionSpec as P

MESH = pl.DeviceIdType.MESH


def weights_kernel(sizes, *refs):
    groups, n, tps = sizes
    count = 6
    srcs, outs = refs[:count], refs[count:2 * count]
    local_sem, send_sem, recv_sem, pass_send, pass_recv = refs[2 * count:]
    grp, fs, tp = lax.axis_index("grp"), lax.axis_index("fs"), lax.axis_index("tp")
    band = n // tps

    def at(g, f, t):
        return {"grp": g, "fs": f, "tp": t}

    barrier = pltpu.get_barrier_semaphore()
    for o in range(n):
        for x in range(tps):
            if o or x:
                pl.semaphore_signal(
                    barrier, inc=1, device_id=at(grp, lax.rem(fs + o, n), lax.rem(tp + x, tps)), device_id_type=MESH
                )
    for y in range(1, groups):
        pl.semaphore_signal(barrier, inc=1, device_id=at(lax.rem(grp + y, groups), fs, tp), device_id_type=MESH)
    pl.semaphore_wait(barrier, n * tps - 1 + groups - 1)

    def src_of(k, peer, share):
        held = outs[k].shape[0]
        first = peer * held if srcs[k].shape[0] > held else 0
        if k in (0, 1, 3, 4):
            part = srcs[k].shape[1] // groups
            return srcs[k].at[pl.ds(first, held), pl.ds(pl.multiple_of(share * part, part), part), :]
        part = srcs[k].shape[2] // groups
        return srcs[k].at[pl.ds(first, held), :, pl.ds(pl.multiple_of(share * part, part), part)]

    def dst_of(k, source, source_tp, share):
        if k in (0, 1, 3, 4):
            rows = srcs[k].shape[1]
            part = rows // groups
            return outs[k].at[:, pl.ds(pl.multiple_of(source * rows + share * part, part), part), :]
        rows, cols = srcs[k].shape[1:]
        part = cols // groups
        return outs[k].at[
            :,
            pl.ds(pl.multiple_of(lax.rem(source, band) * rows, rows), rows),
            pl.ds(pl.multiple_of(source_tp * cols + share * part, part), part),
        ]

    def over_fs(k, slot, src, dst, where):
        return pltpu.make_async_remote_copy(
            src_ref=src, dst_ref=dst, send_sem=send_sem.at[k, slot[0]], recv_sem=recv_sem.at[k, slot[1]],
            device_id=where, device_id_type=MESH,
        )

    def over_grp(k, slot, block, y):
        return pltpu.make_async_remote_copy(
            src_ref=block, dst_ref=block, send_sem=pass_send.at[k, slot, y - 1], recv_sem=pass_recv.at[k, slot, y - 1],
            device_id=at(lax.rem(grp + y, groups), fs, tp), device_id_type=MESH,
        )

    home = fs // band
    mine = lax.rem(fs, band) * tps + tp
    kept = home == tp

    def own(k, g):
        return pltpu.make_async_copy(src_of(k, fs, g), dst_of(k, fs, tp, g), local_sem.at[k, g])

    def row_send(k, o):
        peer = lax.rem(fs + o, n)
        return over_fs(k, (o, o), src_of(k, peer, grp), dst_of(k, fs, tp, grp), at(grp, peer, tp))

    def down_send(k, o):
        peer = lax.rem(fs + o, n)
        return over_fs(k, (o, mine), src_of(k, peer, grp), dst_of(k, fs, tp, grp), at(grp, peer, home))

    for k in (0, 1, 2, 3, 4, 5):
        for o in range(1, n):
            (down_send if k in (2, 5) else row_send)(k, o).start()
        if k in (2, 5):
            @pl.when(kept)
            def _():
                for g in range(groups):
                    own(k, g).start()

            @pl.when(jnp.logical_not(kept))
            def _():
                down_send(k, 0).start()
        else:
            for g in range(groups):
                own(k, g).start()

    def row_arrived(k, o):
        source = lax.rem(fs + n - o, n)
        block = dst_of(k, source, tp, grp)
        over_fs(k, (o, o), block, block, at(grp, source, tp)).wait_recv()
        return block

    def down_block(k, q, x, share):
        return dst_of(k, tp * band + q, x, share)

    def is_own(q, x):
        return jnp.logical_and(tp * band + q == fs, tp == x)

    def others(k):
        for q in range(band):
            for x in range(tps):
                yield q, x, q * tps + x

    for k in (0, 1, 2, 3, 4, 5):
        if k in (2, 5):
            for q, x, slot in others(k):
                @pl.when(jnp.logical_not(is_own(q, x)))
                def _():
                    block = down_block(k, q, x, grp)
                    over_fs(k, (0, slot), block, block, at(grp, tp * band + q, x)).wait_recv()
                    for y in range(1, groups):
                        over_grp(k, slot, block, y).start()
        else:
            for o in range(1, n):
                block = row_arrived(k, o)
                for y in range(1, groups):
                    over_grp(k, o, block, y).start()

    for k in (0, 1, 2, 3, 4, 5):
        if k in (2, 5):
            for q, x, slot in others(k):
                @pl.when(jnp.logical_not(is_own(q, x)))
                def _():
                    for y in range(1, groups):
                        over_grp(k, slot, down_block(k, q, x, grp), y).wait_send()
                        over_grp(k, slot, down_block(k, q, x, lax.rem(grp + groups - y, groups)), y).wait_recv()
            for o in range(1, n):
                down_send(k, o).wait_send()

            @pl.when(kept)
            def _():
                for g in range(groups):
                    own(k, g).wait()

            @pl.when(jnp.logical_not(kept))
            def _():
                down_send(k, 0).wait_send()
        else:
            for o in range(1, n):
                source = lax.rem(fs + n - o, n)
                for y in range(1, groups):
                    over_grp(k, o, dst_of(k, source, tp, grp), y).wait_send()
                    over_grp(k, o, dst_of(k, source, tp, lax.rem(grp + groups - y, groups)), y).wait_recv()
                row_send(k, o).wait_send()
            for g in range(groups):
                own(k, g).wait()


def move_weights(sizes, gate, up, down, shared_gate, shared_up, shared_down):
    groups, n, tps = sizes
    held = gate.shape[0] // n

    def rows(a, lead):
        return jax.ShapeDtypeStruct((lead, n * a.shape[1], a.shape[2]), jnp.bfloat16)

    def downs(a, lead):
        return jax.ShapeDtypeStruct((lead, n // tps * a.shape[1], tps * a.shape[2]), jnp.bfloat16)

    return pl.pallas_call(
        functools.partial(weights_kernel, sizes),
        out_shape=(
            rows(gate, held), rows(up, held), downs(down, held),
            rows(shared_gate, 1), rows(shared_up, 1), downs(shared_down, 1),
        ),
        in_specs=[pl.BlockSpec(memory_space=pltpu.VMEM)] * 6,
        out_specs=[pl.BlockSpec(memory_space=pl.ANY)] * 6,
        scratch_shapes=[
            pltpu.SemaphoreType.DMA((6, groups)),
            pltpu.SemaphoreType.DMA((6, n)),
            pltpu.SemaphoreType.DMA((6, n)),
            pltpu.SemaphoreType.DMA((6, n, groups - 1)),
            pltpu.SemaphoreType.DMA((6, n, groups - 1)),
        ],
        compiler_params=pltpu.CompilerParams(
            collective_id=0, has_side_effects=True, vmem_limit_bytes=16 * 1024 * 1024
        ),
        cost_estimate=pl.CostEstimate(flops=400_000_000, bytes_accessed=20_000_000, transcendentals=0),
    )(gate, up, down, shared_gate, shared_up, shared_down)


def per_device(
    sizes,
    tokens,
    routes,
    route_weights,
    norm_gain,
    gate_experts,
    up_experts,
    down_experts,
    shared_gate,
    shared_up,
    shared_down,
):
    bf16, f32 = jnp.bfloat16, jnp.float32
    groups, n, tps = sizes
    width = tokens.shape[1] * tps
    experts_all = gate_experts.shape[0]
    held = experts_all // n
    gain_rows = norm_gain[None, :, None]
    moved = move_weights(
        sizes,
        (gate_experts * gain_rows).astype(bf16),
        (up_experts * gain_rows).astype(bf16),
        down_experts.astype(bf16),
        (shared_gate[None] * gain_rows).astype(bf16),
        (shared_up[None] * gain_rows).astype(bf16),
        shared_down[None].astype(bf16),
    )
    gate_local, up_local, down_local, sg, su, sd = moved
    sg, su, sd = sg[0], su[0], sd[0]

    gathered = lax.all_gather(tokens, "tp", axis=1, tiled=True)
    widened = gathered.astype(f32)
    normed = (widened * lax.rsqrt(jnp.mean(widened * widened, axis=1, keepdims=True) + 1e-06)).astype(bf16)
    chosen = routes[:, :, None] == jnp.arange(experts_all, dtype=jnp.int32)[None, None, :]
    per_expert = jnp.sum(jnp.where(chosen, route_weights[:, :, None], 0.0), axis=1)
    high = lax.reduce_precision(per_expert, 8, 7)
    pad = -(2 * experts_all) % 128
    packed = jnp.concatenate(
        [normed, high.astype(bf16), (per_expert - high).astype(bf16), jnp.zeros((normed.shape[0], pad), bf16)], axis=1
    )
    everyone = lax.all_gather(packed, "fs", axis=0, tiled=True)
    rows = everyone[:, :width]
    first = lax.axis_index("fs") * held
    scale = lax.dynamic_slice_in_dim(everyone, width + first, held, 1).astype(f32) + lax.dynamic_slice_in_dim(
        everyone, width + experts_all + first, held, 1
    ).astype(f32)

    def hidden(x, g, u):
        return jax.nn.silu(jnp.dot(x, g, preferred_element_type=f32)) * jnp.dot(x, u, preferred_element_type=f32)

    active = jnp.concatenate(
        [(hidden(rows, gate_local[j], up_local[j]) * scale[:, j:j + 1]).astype(bf16) for j in range(held)], axis=1
    )
    partial = jnp.dot(active, down_local.reshape(-1, width), preferred_element_type=f32).astype(bf16)
    own_rows = lax.psum_scatter(partial, "fs", scatter_dimension=0, tiled=True)
    shared_part = jnp.dot(hidden(normed, sg, su).astype(bf16), sd, preferred_element_type=f32)
    both = (own_rows.astype(f32) + shared_part).astype(bf16)
    mixed = lax.psum_scatter(both, "tp", scatter_dimension=1, tiled=True)
    return mixed, gate_local, up_local, down_local, sg, su, sd


def solution(mesh):
    sizes = (mesh.shape["grp"], mesh.shape["fs"], mesh.shape["tp"])
    return jax.shard_map(
        functools.partial(per_device, sizes),
        mesh=mesh,
        in_specs=(
            P(("grp", "fs"), "tp"),
            P(("grp", "fs"), None),
            P(("grp", "fs"), None),
            P("fs"),
            P(None, "fs", "tp"),
            P(None, "fs", "tp"),
            P(None, "fs", "tp"),
            P("fs", "tp"),
            P("fs", "tp"),
            P("fs", "tp"),
        ),
        out_specs=(
            P(("grp", "fs"), "tp"),
            P(("grp", "fs"), None, "tp"),
            P(("grp", "fs"), None, "tp"),
            P(("grp", "fs"), "tp", None),
            P("grp", "tp"),
            P("grp", "tp"),
            P(("grp", "tp"), None),
        ),
        check_vma=False,
    )
```

```python
import functools

import jax
import jax.numpy as jnp
from jax import lax
from jax.experimental import pallas as pl
from jax.experimental.pallas import tpu as pltpu
from jax.sharding import PartitionSpec as P

MESH = pl.DeviceIdType.MESH


def weights_kernel(sizes, *refs):
    groups, n, tps = sizes
    count = 6
    srcs, outs = refs[:count], refs[count:2 * count]
    local_sem, send_sem, recv_sem, pass_send, pass_recv = refs[2 * count:]
    grp, fs, tp = lax.axis_index("grp"), lax.axis_index("fs"), lax.axis_index("tp")
    band = n // tps

    def at(g, f, t):
        return {"grp": g, "fs": f, "tp": t}

    barrier = pltpu.get_barrier_semaphore()
    for o in range(n):
        for x in range(tps):
            if o or x:
                pl.semaphore_signal(
                    barrier, inc=1, device_id=at(grp, lax.rem(fs + o, n), lax.rem(tp + x, tps)), device_id_type=MESH
                )
    for y in range(1, groups):
        pl.semaphore_signal(barrier, inc=1, device_id=at(lax.rem(grp + y, groups), fs, tp), device_id_type=MESH)
    pl.semaphore_wait(barrier, n * tps - 1 + groups - 1)

    def src_of(k, peer, share):
        held = outs[k].shape[0]
        first = peer * held if srcs[k].shape[0] > held else 0
        if k in (0, 1, 3, 4):
            part = srcs[k].shape[1] // groups
            return srcs[k].at[pl.ds(first, held), pl.ds(pl.multiple_of(share * part, part), part), :]
        part = srcs[k].shape[2] // groups
        return srcs[k].at[pl.ds(first, held), :, pl.ds(pl.multiple_of(share * part, part), part)]

    def dst_of(k, source, source_tp, share):
        if k in (0, 1, 3, 4):
            rows = srcs[k].shape[1]
            part = rows // groups
            return outs[k].at[:, pl.ds(pl.multiple_of(source * rows + share * part, part), part), :]
        rows, cols = srcs[k].shape[1:]
        part = cols // groups
        return outs[k].at[
            :,
            pl.ds(pl.multiple_of(lax.rem(source, band) * rows, rows), rows),
            pl.ds(pl.multiple_of(source_tp * cols + share * part, part), part),
        ]

    def over_fs(k, slot, src, dst, where):
        return pltpu.make_async_remote_copy(
            src_ref=src, dst_ref=dst, send_sem=send_sem.at[k, slot[0]], recv_sem=recv_sem.at[k, slot[1]],
            device_id=where, device_id_type=MESH,
        )

    def over_grp(k, slot, block, y):
        return pltpu.make_async_remote_copy(
            src_ref=block, dst_ref=block, send_sem=pass_send.at[k, slot, y - 1], recv_sem=pass_recv.at[k, slot, y - 1],
            device_id=at(lax.rem(grp + y, groups), fs, tp), device_id_type=MESH,
        )

    home = fs // band
    mine = lax.rem(fs, band) * tps + tp
    kept = home == tp

    def own(k, g):
        return pltpu.make_async_copy(src_of(k, fs, g), dst_of(k, fs, tp, g), local_sem.at[k, g])

    def row_send(k, o):
        peer = lax.rem(fs + o, n)
        return over_fs(k, (o, o), src_of(k, peer, grp), dst_of(k, fs, tp, grp), at(grp, peer, tp))

    def down_send(k, o):
        peer = lax.rem(fs + o, n)
        return over_fs(k, (o, mine), src_of(k, peer, grp), dst_of(k, fs, tp, grp), at(grp, peer, home))

    for k in (0, 1, 2, 3, 4, 5):
        for o in range(1, n):
            (down_send if k in (2, 5) else row_send)(k, o).start()
        if k in (2, 5):
            @pl.when(kept)
            def _():
                for g in range(groups):
                    own(k, g).start()

            @pl.when(jnp.logical_not(kept))
            def _():
                down_send(k, 0).start()
        else:
            for g in range(groups):
                own(k, g).start()

    def row_arrived(k, o):
        source = lax.rem(fs + n - o, n)
        block = dst_of(k, source, tp, grp)
        over_fs(k, (o, o), block, block, at(grp, source, tp)).wait_recv()
        return block

    def down_block(k, q, x, share):
        return dst_of(k, tp * band + q, x, share)

    def is_own(q, x):
        return jnp.logical_and(tp * band + q == fs, tp == x)

    def others(k):
        for q in range(band):
            for x in range(tps):
                yield q, x, q * tps + x

    for k in (0, 1, 2, 3, 4, 5):
        if k in (2, 5):
            for q, x, slot in others(k):
                @pl.when(jnp.logical_not(is_own(q, x)))
                def _():
                    block = down_block(k, q, x, grp)
                    over_fs(k, (0, slot), block, block, at(grp, tp * band + q, x)).wait_recv()
                    for y in range(1, groups):
                        over_grp(k, slot, block, y).start()
        else:
            for o in range(1, n):
                block = row_arrived(k, o)
                for y in range(1, groups):
                    over_grp(k, o, block, y).start()

    for k in (0, 1, 2, 3, 4, 5):
        if k in (2, 5):
            for q, x, slot in others(k):
                @pl.when(jnp.logical_not(is_own(q, x)))
                def _():
                    for y in range(1, groups):
                        over_grp(k, slot, down_block(k, q, x, grp), y).wait_send()
                        over_grp(k, slot, down_block(k, q, x, lax.rem(grp + groups - y, groups)), y).wait_recv()
            for o in range(1, n):
                down_send(k, o).wait_send()

            @pl.when(kept)
            def _():
                for g in range(groups):
                    own(k, g).wait()

            @pl.when(jnp.logical_not(kept))
            def _():
                down_send(k, 0).wait_send()
        else:
            for o in range(1, n):
                source = lax.rem(fs + n - o, n)
                for y in range(1, groups):
                    over_grp(k, o, dst_of(k, source, tp, grp), y).wait_send()
                    over_grp(k, o, dst_of(k, source, tp, lax.rem(grp + groups - y, groups)), y).wait_recv()
                row_send(k, o).wait_send()
            for g in range(groups):
                own(k, g).wait()


def move_weights(sizes, gate, up, down, shared_gate, shared_up, shared_down):
    groups, n, tps = sizes
    held = gate.shape[0] // n

    def rows(a, lead):
        return jax.ShapeDtypeStruct((lead, n * a.shape[1], a.shape[2]), jnp.bfloat16)

    def downs(a, lead):
        return jax.ShapeDtypeStruct((lead, n // tps * a.shape[1], tps * a.shape[2]), jnp.bfloat16)

    return pl.pallas_call(
        functools.partial(weights_kernel, sizes),
        out_shape=(
            rows(gate, held), rows(up, held), downs(down, held),
            rows(shared_gate, 1), rows(shared_up, 1), downs(shared_down, 1),
        ),
        in_specs=[pl.BlockSpec(memory_space=pltpu.VMEM)] * 6,
        out_specs=[pl.BlockSpec(memory_space=pl.ANY)] * 6,
        scratch_shapes=[
            pltpu.SemaphoreType.DMA((6, groups)),
            pltpu.SemaphoreType.DMA((6, n)),
            pltpu.SemaphoreType.DMA((6, n)),
            pltpu.SemaphoreType.DMA((6, n, groups - 1)),
            pltpu.SemaphoreType.DMA((6, n, groups - 1)),
        ],
        compiler_params=pltpu.CompilerParams(
            collective_id=0, has_side_effects=True, vmem_limit_bytes=16 * 1024 * 1024
        ),
        cost_estimate=pl.CostEstimate(flops=400_000_000, bytes_accessed=20_000_000, transcendentals=0),
    )(gate, up, down, shared_gate, shared_up, shared_down)


def combine_kernel(sizes, part, shared, out, near, held, across, summed, far, local_sem, near_s, near_r, x_s, x_r, z_s, z_r):
    _, n, tps = sizes
    chips = n // 2
    grp, fs, tp = lax.axis_index("grp"), lax.axis_index("fs"), lax.axis_index("tp")
    chip, core = fs // 2, lax.rem(fs, 2)
    rows, cols = out.shape
    f32 = jnp.float32
    step = 32

    def sibling():
        return {"grp": grp, "fs": chip * 2 + 1 - core, "tp": tp}

    def x_peer(x):
        return {"grp": grp, "fs": fs, "tp": lax.rem(tp + x, tps)}

    def z_peer(o):
        return {"grp": grp, "fs": lax.rem(chip + o, chips) * 2 + core, "tp": tp}

    barrier = pltpu.get_barrier_semaphore()
    peers = [sibling()] + [x_peer(x) for x in range(1, tps)] + [z_peer(o) for o in range(1, chips)]
    for peer in peers:
        pl.semaphore_signal(barrier, inc=1, device_id=peer, device_id_type=MESH)
    pl.semaphore_wait(barrier, len(peers))

    def near_copy(o):
        return pltpu.make_async_remote_copy(
            src_ref=part.at[lax.rem(chip + o, chips) * 2 + 1 - core], dst_ref=near.at[o],
            send_sem=near_s.at[o], recv_sem=near_r.at[o], device_id=sibling(), device_id_type=MESH,
        )

    def keep_copy(o):
        return pltpu.make_async_copy(part.at[lax.rem(chip + o, chips) * 2 + core], held.at[o], local_sem.at[o])

    def x_copy(o, x):
        there = pl.multiple_of(lax.rem(tp + x, tps) * cols, cols)
        return pltpu.make_async_remote_copy(
            src_ref=held.at[o, :, pl.ds(there, cols)], dst_ref=across.at[x - 1, o],
            send_sem=x_s.at[x - 1, o], recv_sem=x_r.at[x - 1, o], device_id=x_peer(x), device_id_type=MESH,
        )

    def z_copy(o):
        return pltpu.make_async_remote_copy(
            src_ref=summed.at[o], dst_ref=far.at[o], send_sem=z_s.at[o], recv_sem=z_r.at[o],
            device_id=z_peer(o), device_id_type=MESH,
        )

    order = list(range(1, chips)) + [0]
    for o in order:
        near_copy(o).start()
        keep_copy(o).start()
    for o in order:
        near_copy(o).wait_recv()
        keep_copy(o).wait()

        @pl.loop(0, rows // step)
        def _(i):
            r = pl.ds(pl.multiple_of(i * step, step), step)
            total = held[o, r, :].astype(f32) + near[o, r, :].astype(f32)
            if o == 0:
                total = total + shared[r, :]
            held[o, r, :] = total.astype(jnp.bfloat16)

        for x in range(1, tps):
            x_copy(o, x).start()
    here = pl.ds(pl.multiple_of(tp * cols, cols), cols)
    for o in order:
        for x in range(1, tps):
            x_copy(o, x).wait_recv()

        @pl.loop(0, rows // step)
        def _(i):
            r = pl.ds(pl.multiple_of(i * step, step), step)
            total = held[o, r, here].astype(f32)
            for x in range(1, tps):
                total = total + across[x - 1, o, r, :].astype(f32)
            summed[o, r, :] = total.astype(jnp.bfloat16)

        if o:
            z_copy(o).start()
    for o in range(1, chips):
        z_copy(o).wait_recv()

    @pl.loop(0, rows // step)
    def _(i):
        r = pl.ds(pl.multiple_of(i * step, step), step)
        total = summed[0, r, :].astype(f32)
        for o in range(1, chips):
            total = total + far[o, r, :].astype(f32)
        out[r, :] = total.astype(jnp.bfloat16)

    for o in order:
        near_copy(o).wait_send()
        for x in range(1, tps):
            x_copy(o, x).wait_send()
        if o:
            z_copy(o).wait_send()


def combine(sizes, partial, shared_part):
    _, n, tps = sizes
    chips = n // 2
    rows, width = shared_part.shape
    cols = width // tps
    bf16 = jnp.bfloat16
    dma = pltpu.SemaphoreType.DMA
    return pl.pallas_call(
        functools.partial(combine_kernel, sizes),
        out_shape=jax.ShapeDtypeStruct((rows, cols), bf16),
        in_specs=[pl.BlockSpec(memory_space=pl.ANY), pl.BlockSpec(memory_space=pltpu.VMEM)],
        out_specs=pl.BlockSpec(memory_space=pltpu.VMEM),
        scratch_shapes=[
            pltpu.VMEM((chips, rows, width), bf16),
            pltpu.VMEM((chips, rows, width), bf16),
            pltpu.VMEM((tps - 1, chips, rows, cols), bf16),
            pltpu.VMEM((chips, rows, cols), bf16),
            pltpu.VMEM((chips, rows, cols), bf16),
            dma((chips,)), dma((chips,)), dma((chips,)),
            dma((tps - 1, chips)), dma((tps - 1, chips)), dma((chips,)), dma((chips,)),
        ],
        compiler_params=pltpu.CompilerParams(
            collective_id=1, has_side_effects=True, vmem_limit_bytes=min(60, 8 + 16 * chips * rows * width // 2**20 // 2) * 2**20
        ),
        cost_estimate=pl.CostEstimate(flops=200_000_000, bytes_accessed=20_000_000, transcendentals=0),
    )(partial.reshape(n, rows, width), shared_part)


def per_device(
    sizes,
    tokens,
    routes,
    route_weights,
    norm_gain,
    gate_experts,
    up_experts,
    down_experts,
    shared_gate,
    shared_up,
    shared_down,
):
    bf16, f32 = jnp.bfloat16, jnp.float32
    groups, n, tps = sizes
    width = tokens.shape[1] * tps
    experts_all = gate_experts.shape[0]
    held = experts_all // n
    gain_rows = norm_gain[None, :, None]
    moved = move_weights(
        sizes,
        (gate_experts * gain_rows).astype(bf16),
        (up_experts * gain_rows).astype(bf16),
        down_experts.astype(bf16),
        (shared_gate[None] * gain_rows).astype(bf16),
        (shared_up[None] * gain_rows).astype(bf16),
        shared_down[None].astype(bf16),
    )
    gate_local, up_local, down_local, sg, su, sd = moved
    sg, su, sd = sg[0], su[0], sd[0]

    gathered = lax.all_gather(tokens, "tp", axis=1, tiled=True)
    widened = gathered.astype(f32)
    normed = (widened * lax.rsqrt(jnp.mean(widened * widened, axis=1, keepdims=True) + 1e-06)).astype(bf16)
    chosen = routes[:, :, None] == jnp.arange(experts_all, dtype=jnp.int32)[None, None, :]
    per_expert = jnp.sum(jnp.where(chosen, route_weights[:, :, None], 0.0), axis=1)
    high = lax.reduce_precision(per_expert, 8, 7)
    pad = -(2 * experts_all) % 128
    packed = jnp.concatenate(
        [normed, high.astype(bf16), (per_expert - high).astype(bf16), jnp.zeros((normed.shape[0], pad), bf16)], axis=1
    )
    everyone = lax.all_gather(packed, "fs", axis=0, tiled=True)
    rows = everyone[:, :width]
    first = lax.axis_index("fs") * held
    scale = lax.dynamic_slice_in_dim(everyone, width + first, held, 1).astype(f32) + lax.dynamic_slice_in_dim(
        everyone, width + experts_all + first, held, 1
    ).astype(f32)

    def hidden(x, g, u):
        return jax.nn.silu(jnp.dot(x, g, preferred_element_type=f32)) * jnp.dot(x, u, preferred_element_type=f32)

    active = jnp.concatenate(
        [(hidden(rows, gate_local[j], up_local[j]) * scale[:, j:j + 1]).astype(bf16) for j in range(held)], axis=1
    )
    partial = jnp.dot(active, down_local.reshape(-1, width), preferred_element_type=f32).astype(bf16)
    shared_part = jnp.dot(hidden(normed, sg, su).astype(bf16), sd, preferred_element_type=f32)
    mixed = combine(sizes, partial, shared_part)
    return mixed, gate_local, up_local, down_local, sg, su, sd


def solution(mesh):
    sizes = (mesh.shape["grp"], mesh.shape["fs"], mesh.shape["tp"])
    return jax.shard_map(
        functools.partial(per_device, sizes),
        mesh=mesh,
        in_specs=(
            P(("grp", "fs"), "tp"),
            P(("grp", "fs"), None),
            P(("grp", "fs"), None),
            P("fs"),
            P(None, "fs", "tp"),
            P(None, "fs", "tp"),
            P(None, "fs", "tp"),
            P("fs", "tp"),
            P("fs", "tp"),
            P("fs", "tp"),
        ),
        out_specs=(
            P(("grp", "fs"), "tp"),
            P(("grp", "fs"), None, "tp"),
            P(("grp", "fs"), None, "tp"),
            P(("grp", "fs"), "tp", None),
            P("grp", "tp"),
            P("grp", "tp"),
            P(("grp", "tp"), None),
        ),
        check_vma=False,
    )
```
